32 devices in a mesh: sp: 8 (over z, y), tp: 4 (over x, core).
Axes of the slice: x: 2, y: 2, z: 4, core: 2. Of those that a mesh axis runs over, the one named last changes fastest.
Arguments:
- query_nope: bfloat16 [1536, 4096], P('sp', 'tp'), may hold values from -6 to 6
- query_rope: bfloat16 [1536, 2048], P('sp', 'tp'), may hold values from -24 to 24
- latent: bfloat16 [1536, 512], P('sp'), may hold values from -6 to 6
- key_rope: bfloat16 [1536, 32], P('sp'), may hold values from -24 to 24
- latent_gain: float32 [512], replicated, may hold values from 0.1 to 1.9
- key_up: bfloat16 [512, 4096], P(None, 'tp'), may hold values from -0.25 to 0.25
- value_up: bfloat16 [512, 4096], P(None, 'tp'), may hold values from -0.25 to 0.25
- out_proj: bfloat16 [4096, 4096], P('tp'), may hold values from -0.09375 to 0.09375
- resid: bfloat16 [1536, 4096], P(('sp', 'tp')), may hold values from -6 to 6
- attn_gain: float32 [4096], replicated, may hold values from 0.1 to 1.9
- pre_gain: float32 [4096], replicated, may hold values from 0.1 to 1.9
- routes: int32 [1536, 2], P(('sp', 'tp')), may hold values from 0 to 7, all different within a row; in each aligned block of 48 rows (0 to 47, 48 to 95, ...) at most 24 rows name the same one
- route_weights: float32 [1536, 2], P(('sp', 'tp')), may hold values from 0.2 to 2
- expert_gate: bfloat16 [8, 4096, 1024], P('sp', None, 'tp'), may hold values from -0.09375 to 0.09375
- expert_up: bfloat16 [8, 4096, 1024], P('sp', None, 'tp'), may hold values from -0.09375 to 0.09375
- expert_down: bfloat16 [8, 1024, 4096], P('sp', 'tp'), may hold values from -0.1875 to 0.1875
- shared_gate: bfloat16 [4096, 1024], P(None, 'tp'), may hold values from -0.09375 to 0.09375
- shared_up: bfloat16 [4096, 1024], P(None, 'tp'), may hold values from -0.09375 to 0.09375
- shared_down: bfloat16 [1024, 4096], P('tp'), may hold values from -0.1875 to 0.1875
- moe_gain: float32 [4096], replicated, may hold values from 0.1 to 1.9
Outputs:
- output: bfloat16 [1536, 4096], P(('sp', 'tp'))
The draws below stay inside these ranges and needn't reach their ends.
Inputs may be any that keep to these rules, and one draw needn't show every extreme that they name: `routes`: A row names 2 different experts. In each aligned block of 48 rows no expert is named by more than 24 rows, and in some block an expert is named by exactly 24 rows.
All inputs are finite; a program needn't handle non-finite values.
Results may differ from the reference program's by a relative error of at most 0.018.
Values may be sent and summed in bfloat16 or wider, within the bound.
A program may use at most 128 MiB of HBM per device.

```python
import math
import jax
import jax.numpy as jnp
import numpy as np
from jax import lax

MODEL_DIM = 4096
HEADS = 64
NOPE_DIM = 64
ROPE_DIM = 32
VALUE_DIM = 64
LATENT = 512
EXPERT_FF = 1024
SHARED_FF = 1024
TOP_K = 2
ROW_DEV = 48
SEQ_LEN = 1536
EXPERTS = 8
CAPACITY = 24
N_TP = 4


def draw_query_rope(key, part):
    drawn_values = jnp.clip(jax.random.normal(jax.random.fold_in(key, 21), (SEQ_LEN, HEADS * ROPE_DIM), jnp.float32), -6.0, 6.0)
    return drawn_values.astype(jnp.bfloat16)


def draw_key_rope(key, part):
    drawn_values = jnp.clip(jax.random.normal(jax.random.fold_in(key, 22), (SEQ_LEN, ROPE_DIM), jnp.float32), -6.0, 6.0)
    return drawn_values.astype(jnp.bfloat16)


def steps_of(rng, extent, pieces, smallest, largest):
    gain = 1.0
    for dim, parts in pieces:
        draws = jax.random.uniform(jax.random.fold_in(jax.random.fold_in(rng, 6), dim), (parts,), jnp.float32, smallest / len(pieces), largest / len(pieces))
        gain = gain * jnp.repeat(jnp.exp(draws), extent[dim] // parts).reshape((-1,) + (1,) * (len(extent) - 1 - dim))
    return gain


def assign_block(stream_key, own, number, rows, amount, top, most, lean):
    ranking = jax.random.permutation(stream_key, amount)
    heavy_load, usual = load_shares(amount, rows * top, most, lean, True), load_shares(amount, rows * top, most, lean, False)
    places = jnp.arange(amount)

    def named(sizes, offset_by):
        used = int((sizes > 0).sum())
        fixed = max(1, used // 4)
        passed = fixed + (places - fixed + offset_by * (used - fixed)) % max(1, amount - fixed)
        return jnp.zeros((amount,), jnp.int32).at[ranking[jnp.where(places < fixed, places, passed)]].set(jnp.asarray(sizes, jnp.int32))

    sizes = jnp.where(number % 4 == 0, named(heavy_load, number // 4), named(usual, number - number // 4 - 1))
    mixed = jax.random.permutation(jax.random.fold_in(own, 3), amount)
    donor, taker = mixed[0:amount // 2 * 2:2], mixed[1:amount // 2 * 2:2]
    room = jnp.minimum(sizes[donor] - 1, most - sizes[taker]) // 2
    room = jnp.where((donor == ranking[0]) | (taker == ranking[0]) | (sizes[taker] == 0), 0, jnp.maximum(room, 0))
    passed = jax.random.randint(jax.random.fold_in(own, 4), (amount // 2,), 0, 1 << 20) % (room + 1)
    sizes = sizes.at[donor].add(-passed).at[taker].add(passed)
    items = jnp.searchsorted(jnp.cumsum(sizes), jnp.arange(rows * top), side="right").astype(jnp.int32)
    table = items.reshape(top, rows).T
    table = table[jax.random.permutation(jax.random.fold_in(own, 1), rows)]
    offset_by = jax.random.randint(jax.random.fold_in(own, 2), (rows, 1), 0, top)
    return jnp.take_along_axis(table, (jnp.arange(top)[None, :] + offset_by) % top, axis=1)


def load_shares(amount, total, reach, slope, full):
    weights = [(1 << 20) // math.isqrt(standing ** slope) + 1 for standing in range(1, amount + 1)]
    largest = reach if full else min(reach, max(-(-total // amount), total * weights[0] // sum(weights)))
    least = 1 if total - largest >= amount - 1 else 0
    counts, spare = [largest] + [least] * (amount - 1), total - largest - least * (amount - 1)
    while spare > 0:
        candidates = [i for i in range(1, amount) if counts[i] < largest] or [i for i in range(1, amount) if counts[i] < reach]
        mass, remaining = sum([weights[i] for i in candidates]), spare
        for i in candidates:
            extra = min(reach - counts[i], max(1, remaining * weights[i] // mass), spare)
            counts[i] = counts[i] + extra
            spare = spare - extra
    return np.array(counts)


def normal_values(own_key, dims, width, reach, pieces=(), kind=jnp.bfloat16):
    array = jax.random.normal(own_key, dims, jnp.float32) * width
    if len(pieces) > 0:
        array = steps_of(own_key, dims, pieces, -0.22, 0.18) * array
    return jnp.clip(array, min=-reach, max=reach).astype(kind)


def setup_inputs(seed: int = 0) -> dict:
    seeds = jax.random.split(jax.random.key(seed), 21)
    query_nope = normal_values(seeds[0], (SEQ_LEN, HEADS * NOPE_DIM), 1.0, 6.0, ((0, 8), (1, 4)))
    query_rope = draw_query_rope(jax.random.fold_in(seeds[20], 71), 0)
    latent = normal_values(seeds[2], (SEQ_LEN, LATENT), 1.0, 6.0, ((0, 8),))
    key_rope = draw_key_rope(jax.random.fold_in(seeds[20], 71), 0)
    latent_gain = jnp.clip(1.0 + 0.18 * jax.random.normal(seeds[4], (LATENT,), jnp.float32), 0.1, 1.9)
    key_up = normal_values(seeds[5], (LATENT, HEADS * NOPE_DIM), LATENT ** -0.5, 0.25, ((1, 4),))
    value_up = normal_values(seeds[6], (LATENT, HEADS * VALUE_DIM), LATENT ** -0.5, 0.25, ((1, 4),))
    out_proj = normal_values(seeds[7], (HEADS * VALUE_DIM, MODEL_DIM), (HEADS * VALUE_DIM) ** -0.5, 0.09375, ((0, 4),))
    resid = normal_values(seeds[8], (SEQ_LEN, MODEL_DIM), 1.0, 6.0, ((0, 32),))
    attn_gain = jnp.clip(1.0 + 0.18 * jax.random.normal(seeds[9], (MODEL_DIM,), jnp.float32), 0.1, 1.9)
    pre_gain = jnp.clip(1.0 + 0.18 * jax.random.normal(seeds[10], (MODEL_DIM,), jnp.float32), 0.1, 1.9)
    routes_keys = jax.random.split(jax.random.fold_in(seeds[11], 1), SEQ_LEN // ROW_DEV)
    routes_turns = jax.random.permutation(jax.random.fold_in(seeds[11], 3), SEQ_LEN // ROW_DEV)
    routes = jax.vmap(lambda own, number: assign_block(jax.random.fold_in(seeds[11], 2), own, number, ROW_DEV, EXPERTS, TOP_K, CAPACITY, 2))(routes_keys, routes_turns).reshape((SEQ_LEN, TOP_K))
    route_weights = jnp.clip(jnp.exp(math.log(2.0) - 2.3025851 * jax.random.uniform(seeds[12], (SEQ_LEN, TOP_K), jnp.float32) ** steps_of(seeds[12], (SEQ_LEN, TOP_K), ((0, 32),), -0.2, 0.2)), 0.2, 2.0)
    expert_gate = normal_values(seeds[13], (EXPERTS, MODEL_DIM, EXPERT_FF), MODEL_DIM ** -0.5, 0.09375, ((0, 8), (2, 4)))
    expert_up = normal_values(seeds[14], (EXPERTS, MODEL_DIM, EXPERT_FF), MODEL_DIM ** -0.5, 0.09375, ((0, 8), (2, 4)))
    expert_down = normal_values(seeds[15], (EXPERTS, EXPERT_FF, MODEL_DIM), EXPERT_FF ** -0.5, 0.1875, ((0, 8), (1, 4)))
    shared_gate = normal_values(seeds[16], (MODEL_DIM, SHARED_FF), MODEL_DIM ** -0.5, 0.09375, ((1, 4),))
    shared_up = normal_values(seeds[17], (MODEL_DIM, SHARED_FF), MODEL_DIM ** -0.5, 0.09375, ((1, 4),))
    shared_down = normal_values(seeds[18], (SHARED_FF, MODEL_DIM), SHARED_FF ** -0.5, 0.1875, ((0, 4),))
    moe_gain = jnp.clip(1.0 + 0.18 * jax.random.normal(seeds[19], (MODEL_DIM,), jnp.float32), 0.1, 1.9)
    return dict(query_nope=query_nope, query_rope=query_rope, latent=latent, key_rope=key_rope, latent_gain=latent_gain, key_up=key_up, value_up=value_up, out_proj=out_proj, resid=resid, attn_gain=attn_gain, pre_gain=pre_gain, routes=routes, route_weights=route_weights, expert_gate=expert_gate, expert_up=expert_up, expert_down=expert_down, shared_gate=shared_gate, shared_up=shared_up, shared_down=shared_down, moe_gain=moe_gain)


epsilon = 1e-06
theta_base = 10000.0

def rms_scale(values, gain_vector):
    return values * lax.rsqrt(lax.optimization_barrier(jnp.mean(values * values, axis=-1, keepdims=True)) + epsilon) * gain_vector

def rotate(values, positions):
    half_dim = values.shape[-1] // 2
    inverse = theta_base ** (-jnp.arange(half_dim, dtype=jnp.float32) / half_dim)
    angles = positions.astype(jnp.float32)[..., None] * inverse
    cosine = jnp.cos(angles)
    sine_part = jnp.sin(angles)
    first_half = values[..., :half_dim]
    second_half = values[..., half_dim:]
    return jnp.concatenate([first_half * cosine - second_half * sine_part, second_half * cosine + first_half * sine_part], axis=-1)

def quarter_product(left_rows, right_cols):
    part_cols = left_rows.shape[1] // N_TP
    result = jnp.zeros((left_rows.shape[0], right_cols.shape[1]), jnp.float32)
    for quarter in range(N_TP):
        partial_value = jnp.dot(left_rows[:, quarter * part_cols:(quarter + 1) * part_cols], right_cols[quarter * part_cols:(quarter + 1) * part_cols], preferred_element_type=jnp.float32)
        rounded = lax.optimization_barrier(partial_value.astype(jnp.bfloat16))
        result = result + rounded.astype(jnp.float32)
    return result

def reference(query_nope, query_rope, latent, key_rope, latent_gain, key_up, value_up, out_proj, resid, attn_gain, pre_gain, routes, route_weights, expert_gate, expert_up, expert_down, shared_gate, shared_up, shared_down, moe_gain):
    positions = jnp.arange(SEQ_LEN, dtype=jnp.int32)
    query_rot = rotate(query_rope.astype(jnp.float32).reshape(SEQ_LEN, HEADS, ROPE_DIM), positions[:, None]).astype(jnp.bfloat16)
    key_rot = rotate(key_rope.astype(jnp.float32), positions).astype(jnp.bfloat16)
    latent_normed = rms_scale(latent.astype(jnp.float32), latent_gain).astype(jnp.bfloat16)
    keys_all = jnp.dot(latent_normed, key_up, preferred_element_type=jnp.float32).astype(jnp.bfloat16)
    keys_all = keys_all.reshape(SEQ_LEN, HEADS, NOPE_DIM).astype(jnp.float32)
    values_all = jnp.dot(latent_normed, value_up, preferred_element_type=jnp.float32).astype(jnp.bfloat16)
    values_all = values_all.reshape(SEQ_LEN, HEADS, VALUE_DIM).astype(jnp.float32)
    query_heads = query_nope.reshape(SEQ_LEN, HEADS, NOPE_DIM).astype(jnp.float32)
    query_rot_f = query_rot.astype(jnp.float32)
    key_rot_f = key_rot.astype(jnp.float32)
    score_scale = (NOPE_DIM + ROPE_DIM) ** (-0.5)
    block_rows = math.gcd(SEQ_LEN, 256)
    outputs = []
    for first_row in range(0, SEQ_LEN, block_rows):
        last_row = first_row + block_rows
        scores = (jnp.einsum('qhd,khd->hqk', query_heads[first_row:last_row], keys_all[:last_row]) + jnp.einsum('qhr,kr->hqk', query_rot_f[first_row:last_row], key_rot_f[:last_row])) * score_scale
        allowed = jnp.arange(last_row)[None, :] <= (first_row + jnp.arange(block_rows))[:, None]
        scores = jnp.where(allowed[None], scores, -jnp.inf)
        row_max = lax.optimization_barrier(jnp.max(scores, axis=-1, keepdims=True))
        exponent = jnp.exp(scores - row_max)
        weights = exponent.astype(jnp.bfloat16).astype(jnp.float32)
        summed = jnp.einsum('hqk,khd->hqd', weights, values_all[:last_row])
        normalized = summed / lax.optimization_barrier(jnp.sum(exponent, axis=-1, keepdims=True))
        outputs.append(normalized.transpose(1, 0, 2).reshape(block_rows, HEADS * VALUE_DIM))
    attention = jnp.concatenate(outputs, axis=0).astype(jnp.bfloat16)
    projected = quarter_product(attention, out_proj)
    mixed = (resid.astype(jnp.float32) + rms_scale(projected, attn_gain)).astype(jnp.bfloat16)
    normed = rms_scale(mixed.astype(jnp.float32), pre_gain).astype(jnp.bfloat16)
    shared_hidden = (jax.nn.silu(jnp.dot(normed, shared_gate, preferred_element_type=jnp.float32)) * jnp.dot(normed, shared_up, preferred_element_type=jnp.float32)).astype(jnp.bfloat16)
    shared_out = quarter_product(shared_hidden, shared_down)
    blocks = SEQ_LEN // ROW_DEV
    flat_routes = routes.reshape(blocks, ROW_DEV * TOP_K)
    onehot = (flat_routes[..., None] == jnp.arange(EXPERTS, dtype=jnp.int32)[None, None, :]).astype(jnp.int32)
    earlier = jnp.cumsum(onehot, axis=1) - onehot
    slot_index = lax.optimization_barrier(jnp.sum(earlier * onehot, axis=-1))
    target = ((jnp.arange(blocks, dtype=jnp.int32)[:, None] * EXPERTS + flat_routes) * CAPACITY + slot_index).reshape(-1)
    source = jnp.arange(SEQ_LEN * TOP_K, dtype=jnp.int32) // TOP_K
    slot_table = jnp.zeros((blocks * EXPERTS * CAPACITY, MODEL_DIM), jnp.bfloat16).at[target].set(normed[source])
    grouped = slot_table.reshape(blocks, EXPERTS, CAPACITY, MODEL_DIM).transpose(1, 0, 2, 3)
    grouped = grouped.reshape(EXPERTS, blocks * CAPACITY, MODEL_DIM)

    def one_expert(operands):
        expert_in, gate_part, up_part, down_part = operands
        hidden = (jax.nn.silu(jnp.dot(expert_in, gate_part, preferred_element_type=jnp.float32)) * jnp.dot(expert_in, up_part, preferred_element_type=jnp.float32)).astype(jnp.bfloat16)
        return quarter_product(hidden, down_part).astype(jnp.bfloat16)
    expert_rows = lax.map(one_expert, (grouped, expert_gate, expert_up, expert_down))
    returned = expert_rows.reshape(EXPERTS, blocks, CAPACITY, MODEL_DIM).transpose(1, 0, 2, 3)
    returned = returned.reshape(blocks * EXPERTS * CAPACITY, MODEL_DIM)
    picked = returned[target].astype(jnp.float32).reshape(SEQ_LEN, TOP_K, MODEL_DIM)
    routed = lax.optimization_barrier(jnp.sum(picked * route_weights[..., None], axis=1))
    moe = shared_out + routed
    return (mixed.astype(jnp.float32) + rms_scale(moe, moe_gain)).astype(jnp.bfloat16)
```

```python
import functools
import math

import jax
import jax.numpy as jnp
from jax import lax
from jax.experimental import pallas as pl
from jax.experimental.pallas import tpu as pltpu
from jax.sharding import PartitionSpec as P

MODEL_DIM = 4096
NOPE_DIM = 64
ROPE_DIM = 32
VALUE_DIM = 64
TOP_K = 2


epsilon = 1e-06
theta_base = 10000.0


def rms_scale(values, gain_vector):
    return (
        values
        * lax.rsqrt(jnp.mean(values * values, axis=-1, keepdims=True) + epsilon)
        * gain_vector
    )


def rotate(values, positions):
    half_dim = values.shape[-1] // 2
    inverse = theta_base ** (-jnp.arange(half_dim, dtype=jnp.float32) / half_dim)
    angles = positions.astype(jnp.float32)[..., None] * inverse
    cosine = jnp.cos(angles)
    sine_part = jnp.sin(angles)
    first_half = values[..., :half_dim]
    second_half = values[..., half_dim:]
    return jnp.concatenate(
        [
            first_half * cosine - second_half * sine_part,
            second_half * cosine + first_half * sine_part,
        ],
        axis=-1,
    )


def expert_block(expert_in, gate_part, up_part, down_part):
    hidden = (
        jax.nn.silu(jnp.dot(expert_in, gate_part, preferred_element_type=jnp.float32))
        * jnp.dot(expert_in, up_part, preferred_element_type=jnp.float32)
    ).astype(jnp.bfloat16)
    return jnp.dot(hidden, down_part, preferred_element_type=jnp.float32).astype(jnp.bfloat16)


def remote_copy(source, dest, send_sem, recv_sem, sp_index, tp_index):
    return pltpu.make_async_remote_copy(
        src_ref=source,
        dst_ref=dest,
        send_sem=send_sem,
        recv_sem=recv_sem,
        device_id=(sp_index, tp_index),
        device_id_type=pl.DeviceIdType.MESH,
    )


def enter(me, tp_me, sp_count):
    barrier = pltpu.get_barrier_semaphore()
    for bit in (1, 2):
        pl.semaphore_signal(
            barrier,
            inc=1,
            device_id=(me, flip(tp_me, bit)),
            device_id_type=pl.DeviceIdType.MESH,
        )

    def greet(k, carry):
        pl.semaphore_signal(
            barrier,
            inc=1,
            device_id=(lax.rem(me + 1 + k, sp_count), tp_me),
            device_id_type=pl.DeviceIdType.MESH,
        )
        return carry

    lax.fori_loop(0, sp_count - 1, greet, 0)
    pl.semaphore_wait(barrier, sp_count + 1)


def flip(tp_me, bit):
    high, low = tp_me // 2, lax.rem(tp_me, 2)
    return high * 2 + (1 - low) if bit == 1 else (1 - high) * 2 + low


def add(*parts):
    total = parts[0].astype(jnp.float32)
    for part in parts[1:]:
        total = total + part.astype(jnp.float32)
    return total


class PairSum:
    def __init__(self, parts, got1, half, got2, sems, me, tp_me):
        self.parts, self.got1, self.half, self.got2 = parts, got1, half, got2
        self.sems, self.me, self.tp_me = sems, me, tp_me
        self.high, self.low = tp_me // 2, lax.rem(tp_me, 2)

    def first(self, side, e):
        return remote_copy(
            self.parts.at[side, 1 - self.low, e],
            self.got1.at[side, e],
            self.sems.at[0, side, e],
            self.sems.at[1, side, e],
            self.me,
            flip(self.tp_me, 1),
        )

    def second(self, e):
        return remote_copy(
            self.half.at[e],
            self.got2.at[e],
            self.sems.at[0, 2, e],
            self.sems.at[1, 2, e],
            self.me,
            flip(self.tp_me, 2),
        )

    def start(self, e):
        for side in range(2):
            self.first(side, e).start()

    def middle(self, e):
        for side in range(2):
            self.first(side, e).wait_recv()
        other = 1 - self.high
        self.half[e] = add(self.parts[other, self.low, e], self.got1[other, e]).astype(
            self.half.dtype
        )
        self.second(e).start()

    def finish(self, e):
        self.second(e).wait_recv()
        return add(
            self.parts[self.high, self.low, e], self.got1[self.high, e], self.got2[e]
        )

    def drain(self, e):
        for side in range(2):
            self.first(side, e).wait_send()
        self.second(e).wait_send()


def loop(count, body):
    def step(k, carry):
        body(k)
        return carry

    lax.fori_loop(0, count, step, 0)


def reduce_kernel(parts, out, got1, half, got2, sems):
    me, tp_me = lax.axis_index("sp"), lax.axis_index("tp")
    enter(me, tp_me, 1)
    pair = PairSum(parts, got1, half, got2, sems, me, tp_me)
    pieces = parts.shape[2]
    loop(pieces, pair.start)
    loop(pieces, pair.middle)

    def close(e):
        out[e] = pair.finish(e)

    loop(pieces, close)
    loop(pieces, pair.drain)


def pair_scratch(shape):
    pieces, block = shape[2], tuple(shape[2:])
    return [
        pltpu.VMEM((2,) + block, jnp.bfloat16),
        pltpu.VMEM(block, jnp.bfloat16),
        pltpu.VMEM(block, jnp.bfloat16),
        pltpu.SemaphoreType.DMA((2, 3, pieces)),
    ]


IN_VMEM = pl.BlockSpec(memory_space=pltpu.VMEM)


def comm_params(number):
    return pltpu.CompilerParams(
        collective_id=number, has_side_effects=True, vmem_limit_bytes=60 * 1024 * 1024
    )


def tp_reduce(parts):
    return pl.pallas_call(
        reduce_kernel,
        out_shape=jax.ShapeDtypeStruct(parts.shape[2:], jnp.float32),
        in_specs=[IN_VMEM],
        out_specs=IN_VMEM,
        scratch_shapes=pair_scratch(parts.shape),
        compiler_params=comm_params(0),
    )(parts)


def dispatch_kernel(sp_count, table, normed, column, group, to_sp, to_low, to_high, relay, norm_sems):
    me, tp_me = lax.axis_index("sp"), lax.axis_index("tp")
    low_peer, high_peer = flip(tp_me, 1), flip(tp_me, 2)
    last = sp_count - 1
    enter(me, tp_me, sp_count)

    def source_of(k):
        return lax.rem(me + 2 * sp_count - 1 - k, sp_count)

    def norm_copy(index, source, slot, peer):
        return remote_copy(
            source, group.at[slot], norm_sems.at[0, index], norm_sems.at[1, index], me, peer
        )

    norm_low = norm_copy(0, normed, tp_me, low_peer)
    norm_high = norm_copy(1, normed, tp_me, high_peer)
    norm_relay = norm_copy(2, group.at[high_peer], high_peer, low_peer)
    norm_low.start()
    norm_high.start()

    def spread(k):
        e = lax.rem(me + 1 + k, sp_count)
        return remote_copy(
            table.at[e], column.at[tp_me, me], to_sp.at[0, k], to_sp.at[1, k], e, tp_me
        )

    def forward(sems, k, source, slot, peer):
        return remote_copy(
            source, column.at[slot, source_of(k)], sems.at[0, k], sems.at[1, k], me, peer
        )

    def own_low():
        return forward(to_low, last, table.at[me], tp_me, low_peer)

    def own_high():
        return forward(to_high, last, table.at[me], tp_me, high_peer)

    def low(k):
        return forward(to_low, k, column.at[tp_me, source_of(k)], tp_me, low_peer)

    def high(k):
        return forward(to_high, k, column.at[tp_me, source_of(k)], tp_me, high_peer)

    def relayed(k):
        return forward(relay, k, column.at[high_peer, source_of(k)], high_peer, low_peer)

    own_high().start()
    own_low().start()
    loop(last, lambda k: spread(k).start())
    group[tp_me] = normed[...]
    column[tp_me, me] = table[me]
    norm_high.wait_recv()
    norm_relay.start()

    def arrive(k):
        spread(k).wait_recv()
        high(k).start()
        low(k).start()

    loop(last, arrive)

    def pass_on(k):
        high(k).wait_recv()
        relayed(k).start()

    pass_on(last)
    loop(last, pass_on)

    def settle(k):
        low(k).wait_recv()
        relayed(k).wait_recv()
        relayed(k).wait_send()

    loop(sp_count, settle)

    def sent(k):
        spread(k).wait_send()
        low(k).wait_send()
        high(k).wait_send()

    loop(last, sent)
    own_low().wait_send()
    own_high().wait_send()
    norm_low.wait()
    norm_high.wait_send()
    norm_relay.wait()


def dispatch(table, normed):
    sp_count, tp_count = lax.axis_size("sp"), lax.axis_size("tp")
    ring = pltpu.SemaphoreType.DMA((2, sp_count))
    return pl.pallas_call(
        functools.partial(dispatch_kernel, sp_count),
        out_shape=(
            jax.ShapeDtypeStruct((tp_count,) + table.shape, table.dtype),
            jax.ShapeDtypeStruct((tp_count,) + normed.shape, normed.dtype),
        ),
        in_specs=[IN_VMEM] * 2,
        out_specs=(IN_VMEM, IN_VMEM),
        scratch_shapes=[ring, ring, ring, ring, pltpu.SemaphoreType.DMA((2, 3))],
        compiler_params=comm_params(1),
    )(table, normed)


def return_kernel(
    sp_count,
    parts,
    shared,
    rows_out,
    shared_out,
    got1,
    half,
    got2,
    sems,
    shared_got1,
    shared_half,
    shared_got2,
    shared_sems,
    final,
    back,
):
    me, tp_me = lax.axis_index("sp"), lax.axis_index("tp")
    last = sp_count - 1
    enter(me, tp_me, sp_count)
    routed = PairSum(parts, got1, half, got2, sems, me, tp_me)
    common = PairSum(shared, shared_got1, shared_half, shared_got2, shared_sems, me, tp_me)
    common_pieces = shared.shape[2]

    def owner(k):
        return lax.rem(me + 1 + k, sp_count)

    def home(k):
        e = owner(k)
        return remote_copy(
            final.at[e], rows_out.at[me], back.at[0, k], back.at[1, k], e, tp_me
        )

    loop(sp_count, lambda k: routed.start(owner(k)))
    loop(common_pieces, common.start)
    loop(sp_count, lambda k: routed.middle(owner(k)))
    loop(common_pieces, common.middle)

    def deliver(k):
        e = owner(k)
        final[e] = routed.finish(e).astype(final.dtype)
        home(k).start()

    loop(last, deliver)
    rows_out[me] = routed.finish(me).astype(rows_out.dtype)

    def close(e):
        shared_out[e] = common.finish(e)

    loop(common_pieces, close)
    loop(sp_count, routed.drain)
    loop(common_pieces, common.drain)
    loop(last, lambda k: home(k).wait())


def give_back(parts, shared):
    sp_count = lax.axis_size("sp")
    return pl.pallas_call(
        functools.partial(return_kernel, sp_count),
        out_shape=(
            jax.ShapeDtypeStruct(parts.shape[2:], parts.dtype),
            jax.ShapeDtypeStruct(shared.shape[2:], jnp.float32),
        ),
        in_specs=[IN_VMEM] * 2,
        out_specs=(IN_VMEM, IN_VMEM),
        scratch_shapes=pair_scratch(parts.shape)
        + pair_scratch(shared.shape)
        + [
            pltpu.VMEM(parts.shape[2:], parts.dtype),
            pltpu.SemaphoreType.DMA((2, sp_count)),
        ],
        compiler_params=comm_params(2),
    )(parts, shared)


def dispatch_table(normed_rows, route_rows, route_weights, experts, capacity):
    row_count = normed_rows.shape[0]
    flat_routes = route_rows.reshape(-1)
    onehot = (flat_routes[:, None] == jnp.arange(experts, dtype=jnp.int32)[None, :]).astype(
        jnp.int32
    )
    earlier = jnp.cumsum(onehot, axis=0) - onehot
    target = flat_routes * capacity + jnp.sum(earlier * onehot, axis=1)
    matches = (
        target.reshape(row_count, -1)[None, :, :]
        == jnp.arange(experts * capacity, dtype=jnp.int32)[:, None, None]
    )
    spread = jnp.any(matches, axis=2).astype(jnp.bfloat16)
    slot_table = jnp.dot(spread, normed_rows, preferred_element_type=jnp.float32).astype(
        jnp.bfloat16
    )
    combine = jnp.sum(jnp.where(matches, route_weights[None], 0.0), axis=2).T
    return (slot_table.reshape(experts, capacity, normed_rows.shape[1]), combine)


def on_device(
    query_nope,
    query_rope,
    latent,
    key_rope,
    latent_gain,
    key_up,
    value_up,
    out_proj,
    resid,
    attn_gain,
    pre_gain,
    routes,
    route_weights,
    expert_gate,
    expert_up,
    expert_down,
    shared_gate,
    shared_up,
    shared_down,
    moe_gain,
):
    local_rows = query_nope.shape[0]
    heads_here = query_nope.shape[1] // NOPE_DIM
    query_pos = lax.axis_index("sp") * local_rows + jnp.arange(local_rows, dtype=jnp.int32)
    last_query = lax.axis_index("sp") * local_rows + local_rows - 1
    query_rot = rotate(
        query_rope.astype(jnp.float32).reshape(local_rows, heads_here, ROPE_DIM), query_pos[:, None]
    ).astype(jnp.bfloat16)
    key_rot = rotate(key_rope.astype(jnp.float32), query_pos).astype(jnp.bfloat16)
    latent_normed = rms_scale(latent.astype(jnp.float32), latent_gain).astype(jnp.bfloat16)
    query_heads = query_nope.reshape(local_rows, heads_here, NOPE_DIM)
    score_scale = (NOPE_DIM + ROPE_DIM) ** (-0.5)

    def attend(state_now, latent_rows, rotary_rows, key_start):
        piece_rows = latent_rows.shape[0]
        keys_here = jnp.dot(latent_rows, key_up, preferred_element_type=jnp.float32).astype(
            jnp.bfloat16
        )
        keys_here = keys_here.reshape(piece_rows, heads_here, NOPE_DIM)
        values_here = jnp.dot(latent_rows, value_up, preferred_element_type=jnp.float32).astype(
            jnp.bfloat16
        )
        values_here = values_here.reshape(piece_rows, heads_here, VALUE_DIM)
        scores = (
            jnp.einsum("qhd,khd->hqk", query_heads, keys_here, preferred_element_type=jnp.float32)
            + jnp.einsum("qhr,kr->hqk", query_rot, rotary_rows, preferred_element_type=jnp.float32)
        ) * score_scale
        allowed = (key_start + jnp.arange(piece_rows, dtype=jnp.int32))[None, :] <= query_pos[
            :, None
        ]
        scores = jnp.where(allowed[None], scores, -1e30)
        running, total_sum, summed = state_now
        newest = jnp.maximum(running, jnp.max(scores, axis=-1))
        factor = jnp.exp(running - newest)
        exponent = jnp.exp(scores - newest[..., None])
        total_sum = total_sum * factor + jnp.sum(exponent, axis=-1)
        summed = summed * factor[..., None] + jnp.einsum(
            "hqk,khd->hqd",
            exponent.astype(jnp.bfloat16),
            values_here,
            preferred_element_type=jnp.float32,
        )
        return (newest, total_sum, summed)

    initial = (
        jnp.full((heads_here, local_rows), -1e30, jnp.float32),
        jnp.zeros((heads_here, local_rows), jnp.float32),
        jnp.zeros((heads_here, local_rows, VALUE_DIM), jnp.float32),
    )
    gathered = lax.all_gather(
        jnp.concatenate([latent_normed, key_rot], axis=1), "sp", axis=0, tiled=True
    )
    latent_piece = gathered[:, : latent.shape[1]]
    rotary_piece = gathered[:, latent.shape[1] :]
    piece_rows = latent_piece.shape[0]
    step_rows = math.gcd(piece_rows, 512)

    def one_step(step_index, inner_state):
        offset = step_index * step_rows
        latent_rows = lax.dynamic_slice_in_dim(latent_piece, offset, step_rows, 0)
        rotary_rows = lax.dynamic_slice_in_dim(rotary_piece, offset, step_rows, 0)
        return lax.cond(
            offset <= last_query,
            lambda carried: attend(carried, latent_rows, rotary_rows, offset),
            lambda carried: carried,
            inner_state,
        )

    running, total_sum, summed = lax.fori_loop(0, piece_rows // step_rows, one_step, initial)
    attention = (
        (summed / total_sum[..., None])
        .transpose(1, 0, 2)
        .reshape(local_rows, heads_here * VALUE_DIM)
    )
    attention = attention.astype(jnp.bfloat16)
    rows_here = resid.shape[0]
    model_dim = resid.shape[1]
    piece = math.gcd(rows_here, 16)
    projected = tp_reduce(
        jnp.dot(attention, out_proj, preferred_element_type=jnp.float32)
        .astype(jnp.bfloat16)
        .reshape(2, 2, -1, piece, model_dim)
    ).reshape(rows_here, model_dim)
    mixed = (resid.astype(jnp.float32) + rms_scale(projected, attn_gain)).astype(jnp.bfloat16)
    normed = rms_scale(mixed.astype(jnp.float32), pre_gain).astype(jnp.bfloat16)
    experts = lax.axis_size("sp")
    capacity = max(2, 2 * rows_here * TOP_K // experts)
    own_table, combine = dispatch_table(normed, routes, route_weights, experts, capacity)
    column, group_normed = dispatch(own_table, normed)
    expert_out = expert_block(
        column.reshape(-1, model_dim), expert_gate[0], expert_up[0], expert_down[0]
    )
    shared_part = expert_block(
        group_normed.reshape(-1, model_dim), shared_gate, shared_up, shared_down
    )
    expert_rows, shared_sum = give_back(
        expert_out.reshape(2, 2, experts, capacity, model_dim),
        shared_part.reshape(2, 2, -1, piece, model_dim),
    )
    expert_rows = expert_rows.reshape(-1, model_dim)
    shared_out = shared_sum.reshape(rows_here, model_dim)
    upper = combine.astype(jnp.bfloat16)
    lower = (combine - upper.astype(jnp.float32)).astype(jnp.bfloat16)
    both = jnp.dot(
        jnp.concatenate([upper, lower], axis=0), expert_rows, preferred_element_type=jnp.float32
    )
    routed = both[:rows_here] + both[rows_here:]
    moe = shared_out + routed
    return (mixed.astype(jnp.float32) + rms_scale(moe, moe_gain)).astype(jnp.bfloat16)


def solution(mesh):
    in_specs = (
        P("sp", "tp"),
        P("sp", "tp"),
        P("sp", None),
        P("sp", None),
        P(),
        P(None, "tp"),
        P(None, "tp"),
        P("tp", None),
        P(("sp", "tp"), None),
        P(),
        P(),
        P(("sp", "tp"), None),
        P(("sp", "tp"), None),
        P("sp", None, "tp"),
        P("sp", None, "tp"),
        P("sp", "tp", None),
        P(None, "tp"),
        P(None, "tp"),
        P("tp", None),
        P(),
    )
    out_specs = P(("sp", "tp"), None)
    return jax.shard_map(
        on_device, mesh=mesh, in_specs=in_specs, out_specs=out_specs, check_vma=False
    )
```

```python
import functools
import math

import jax
import jax.numpy as jnp
from jax import lax
from jax.experimental import pallas as pl
from jax.experimental.pallas import tpu as pltpu
from jax.sharding import PartitionSpec as P

MODEL_DIM = 4096
NOPE_DIM = 64
ROPE_DIM = 32
VALUE_DIM = 64
TOP_K = 2


epsilon = 1e-06
theta_base = 10000.0


def rms_scale(values, gain_vector):
    return (
        values
        * lax.rsqrt(jnp.mean(values * values, axis=-1, keepdims=True) + epsilon)
        * gain_vector
    )


def rotate(values, positions):
    half_dim = values.shape[-1] // 2
    inverse = theta_base ** (-jnp.arange(half_dim, dtype=jnp.float32) / half_dim)
    angles = positions.astype(jnp.float32)[..., None] * inverse
    cosine = jnp.cos(angles)
    sine_part = jnp.sin(angles)
    first_half = values[..., :half_dim]
    second_half = values[..., half_dim:]
    return jnp.concatenate(
        [
            first_half * cosine - second_half * sine_part,
            second_half * cosine + first_half * sine_part,
        ],
        axis=-1,
    )


def expert_block(expert_in, gate_part, up_part, down_part):
    hidden = (
        jax.nn.silu(jnp.dot(expert_in, gate_part, preferred_element_type=jnp.float32))
        * jnp.dot(expert_in, up_part, preferred_element_type=jnp.float32)
    ).astype(jnp.bfloat16)
    return jnp.dot(hidden, down_part, preferred_element_type=jnp.float32).astype(jnp.bfloat16)


def remote_copy(source, dest, send_sem, recv_sem, sp_index, tp_index):
    return pltpu.make_async_remote_copy(
        src_ref=source,
        dst_ref=dest,
        send_sem=send_sem,
        recv_sem=recv_sem,
        device_id=(sp_index, tp_index),
        device_id_type=pl.DeviceIdType.MESH,
    )


def enter(me, tp_me, sp_count):
    barrier = pltpu.get_barrier_semaphore()
    for bit in (1, 2):
        pl.semaphore_signal(
            barrier,
            inc=1,
            device_id=(me, flip(tp_me, bit)),
            device_id_type=pl.DeviceIdType.MESH,
        )

    def greet(k, carry):
        pl.semaphore_signal(
            barrier,
            inc=1,
            device_id=(lax.rem(me + 1 + k, sp_count), tp_me),
            device_id_type=pl.DeviceIdType.MESH,
        )
        return carry

    lax.fori_loop(0, sp_count - 1, greet, 0)
    pl.semaphore_wait(barrier, sp_count + 1)


def flip(tp_me, bit):
    high, low = tp_me // 2, lax.rem(tp_me, 2)
    return high * 2 + (1 - low) if bit == 1 else (1 - high) * 2 + low


def add(*parts):
    total = parts[0].astype(jnp.float32)
    for part in parts[1:]:
        total = total + part.astype(jnp.float32)
    return total


class PairSum:
    def __init__(self, parts, got1, half, got2, sems, me, tp_me):
        self.parts, self.got1, self.half, self.got2 = parts, got1, half, got2
        self.sems, self.me, self.tp_me = sems, me, tp_me
        self.high, self.low = tp_me // 2, lax.rem(tp_me, 2)

    def first(self, side, e):
        return remote_copy(
            self.parts.at[side, 1 - self.low, e],
            self.got1.at[side, e],
            self.sems.at[0, side, e],
            self.sems.at[1, side, e],
            self.me,
            flip(self.tp_me, 1),
        )

    def second(self, e):
        return remote_copy(
            self.half.at[e],
            self.got2.at[e],
            self.sems.at[0, 2, e],
            self.sems.at[1, 2, e],
            self.me,
            flip(self.tp_me, 2),
        )

    def start(self, e):
        for side in range(2):
            self.first(side, e).start()

    def middle(self, e):
        for side in range(2):
            self.first(side, e).wait_recv()
        other = 1 - self.high
        self.half[e] = add(self.parts[other, self.low, e], self.got1[other, e]).astype(
            self.half.dtype
        )
        self.second(e).start()

    def finish(self, e):
        self.second(e).wait_recv()
        return add(
            self.parts[self.high, self.low, e], self.got1[self.high, e], self.got2[e]
        )

    def drain(self, e):
        for side in range(2):
            self.first(side, e).wait_send()
        self.second(e).wait_send()


def loop(count, body):
    def step(k, carry):
        body(k)
        return carry

    lax.fori_loop(0, count, step, 0)


def reduce_kernel(parts, out, got1, half, got2, sems):
    me, tp_me = lax.axis_index("sp"), lax.axis_index("tp")
    enter(me, tp_me, 1)
    pair = PairSum(parts, got1, half, got2, sems, me, tp_me)
    pieces = parts.shape[2]
    loop(pieces, pair.start)
    loop(pieces, pair.middle)

    def close(e):
        out[e] = pair.finish(e)

    loop(pieces, close)
    loop(pieces, pair.drain)


def pair_scratch(shape):
    pieces, block = shape[2], tuple(shape[2:])
    return [
        pltpu.VMEM((2,) + block, jnp.bfloat16),
        pltpu.VMEM(block, jnp.bfloat16),
        pltpu.VMEM(block, jnp.bfloat16),
        pltpu.SemaphoreType.DMA((2, 3, pieces)),
    ]


IN_VMEM = pl.BlockSpec(memory_space=pltpu.VMEM)


def comm_params(number):
    return pltpu.CompilerParams(
        collective_id=number, has_side_effects=True, vmem_limit_bytes=60 * 1024 * 1024
    )


def tp_reduce(parts):
    return pl.pallas_call(
        reduce_kernel,
        out_shape=jax.ShapeDtypeStruct(parts.shape[2:], jnp.float32),
        in_specs=[IN_VMEM],
        out_specs=IN_VMEM,
        scratch_shapes=pair_scratch(parts.shape),
        compiler_params=comm_params(0),
    )(parts)


def dispatch_kernel(sp_count, table, normed, column, group, to_sp, to_low, to_high, relay, norm_sems):
    me, tp_me = lax.axis_index("sp"), lax.axis_index("tp")
    low_peer, high_peer = flip(tp_me, 1), flip(tp_me, 2)
    last = sp_count - 1
    enter(me, tp_me, sp_count)

    def source_of(k):
        return lax.rem(me + 2 * sp_count - 1 - k, sp_count)

    def norm_copy(index, source, slot, peer):
        return remote_copy(
            source, group.at[slot], norm_sems.at[0, index], norm_sems.at[1, index], me, peer
        )

    norm_low = norm_copy(0, normed, tp_me, low_peer)
    norm_high = norm_copy(1, normed, tp_me, high_peer)
    norm_relay = norm_copy(2, group.at[high_peer], high_peer, low_peer)
    norm_low.start()
    norm_high.start()

    def spread(k):
        e = lax.rem(me + 1 + k, sp_count)
        return remote_copy(
            table.at[e], column.at[tp_me, me], to_sp.at[0, k], to_sp.at[1, k], e, tp_me
        )

    def forward(sems, k, source, slot, peer):
        return remote_copy(
            source, column.at[slot, source_of(k)], sems.at[0, k], sems.at[1, k], me, peer
        )

    def own_low():
        return forward(to_low, last, table.at[me], tp_me, low_peer)

    def own_high():
        return forward(to_high, last, table.at[me], tp_me, high_peer)

    def low(k):
        return forward(to_low, k, column.at[tp_me, source_of(k)], tp_me, low_peer)

    def high(k):
        return forward(to_high, k, column.at[tp_me, source_of(k)], tp_me, high_peer)

    def relayed(k):
        return forward(relay, k, column.at[high_peer, source_of(k)], high_peer, low_peer)

    own_high().start()
    own_low().start()
    loop(last, lambda k: spread(k).start())
    group[tp_me] = normed[...]
    column[tp_me, me] = table[me]
    norm_high.wait_recv()
    norm_relay.start()

    def arrive(k):
        spread(k).wait_recv()
        high(k).start()
        low(k).start()

    loop(last, arrive)

    def pass_on(k):
        high(k).wait_recv()
        relayed(k).start()

    pass_on(last)
    loop(last, pass_on)

    def settle(k):
        low(k).wait_recv()
        relayed(k).wait_recv()
        relayed(k).wait_send()

    loop(sp_count, settle)

    def sent(k):
        spread(k).wait_send()
        low(k).wait_send()
        high(k).wait_send()

    loop(last, sent)
    own_low().wait_send()
    own_high().wait_send()
    norm_low.wait()
    norm_high.wait_send()
    norm_relay.wait()


def dispatch(table, normed):
    sp_count, tp_count = lax.axis_size("sp"), lax.axis_size("tp")
    ring = pltpu.SemaphoreType.DMA((2, sp_count))
    return pl.pallas_call(
        functools.partial(dispatch_kernel, sp_count),
        out_shape=(
            jax.ShapeDtypeStruct((tp_count,) + table.shape, table.dtype),
            jax.ShapeDtypeStruct((tp_count,) + normed.shape, normed.dtype),
        ),
        in_specs=[IN_VMEM] * 2,
        out_specs=(IN_VMEM, IN_VMEM),
        scratch_shapes=[ring, ring, ring, ring, pltpu.SemaphoreType.DMA((2, 3))],
        compiler_params=comm_params(1),
    )(table, normed)


def return_kernel(
    sp_count,
    parts,
    shared,
    rows_out,
    shared_out,
    got1,
    half,
    got2,
    sems,
    shared_got1,
    shared_half,
    shared_got2,
    shared_sems,
    final,
    back,
):
    me, tp_me = lax.axis_index("sp"), lax.axis_index("tp")
    last = sp_count - 1
    enter(me, tp_me, sp_count)
    routed = PairSum(parts, got1, half, got2, sems, me, tp_me)
    common = PairSum(shared, shared_got1, shared_half, shared_got2, shared_sems, me, tp_me)
    common_pieces = shared.shape[2]

    def owner(k):
        return lax.rem(me + 1 + k, sp_count)

    def home(k):
        e = owner(k)
        return remote_copy(
            final.at[e], rows_out.at[me], back.at[0, k], back.at[1, k], e, tp_me
        )

    loop(sp_count, lambda k: routed.start(owner(k)))
    loop(common_pieces, common.start)
    loop(sp_count, lambda k: routed.middle(owner(k)))
    loop(common_pieces, common.middle)

    def deliver(k):
        e = owner(k)
        final[e] = routed.finish(e).astype(final.dtype)
        home(k).start()

    loop(last, deliver)
    rows_out[me] = routed.finish(me).astype(rows_out.dtype)

    def close(e):
        shared_out[e] = common.finish(e)

    loop(common_pieces, close)
    loop(sp_count, routed.drain)
    loop(common_pieces, common.drain)
    loop(last, lambda k: home(k).wait())


def give_back(parts, shared):
    sp_count = lax.axis_size("sp")
    return pl.pallas_call(
        functools.partial(return_kernel, sp_count),
        out_shape=(
            jax.ShapeDtypeStruct(parts.shape[2:], parts.dtype),
            jax.ShapeDtypeStruct(shared.shape[2:], jnp.float32),
        ),
        in_specs=[IN_VMEM] * 2,
        out_specs=(IN_VMEM, IN_VMEM),
        scratch_shapes=pair_scratch(parts.shape)
        + pair_scratch(shared.shape)
        + [
            pltpu.VMEM(parts.shape[2:], parts.dtype),
            pltpu.SemaphoreType.DMA((2, sp_count)),
        ],
        compiler_params=comm_params(2),
    )(parts, shared)


def gather_kernel(sp_count, block, column, to_sp, to_low, to_high, relay):
    me, tp_me = lax.axis_index("sp"), lax.axis_index("tp")
    low_peer, high_peer = flip(tp_me, 1), flip(tp_me, 2)
    last = sp_count - 1
    enter(me, tp_me, sp_count)

    def source_of(k):
        return lax.rem(me + 2 * sp_count - 1 - k, sp_count)

    def spread(k):
        e = lax.rem(me + 1 + k, sp_count)
        return remote_copy(
            block, column.at[me, tp_me], to_sp.at[0, k], to_sp.at[1, k], e, tp_me
        )

    def forward(sems, k, source, slot, peer):
        return remote_copy(
            source, column.at[source_of(k), slot], sems.at[0, k], sems.at[1, k], me, peer
        )

    def own_low():
        return forward(to_low, last, block, tp_me, low_peer)

    def own_high():
        return forward(to_high, last, block, tp_me, high_peer)

    def low(k):
        return forward(to_low, k, column.at[source_of(k), tp_me], tp_me, low_peer)

    def high(k):
        return forward(to_high, k, column.at[source_of(k), tp_me], tp_me, high_peer)

    def relayed(k):
        return forward(relay, k, column.at[source_of(k), high_peer], high_peer, low_peer)

    loop(last, lambda k: spread(k).start())
    own_high().start()
    own_low().start()
    column[me, tp_me] = block[...]

    def arrive(k):
        spread(k).wait_recv()
        high(k).start()
        low(k).start()

    loop(last, arrive)

    def pass_on(k):
        high(k).wait_recv()
        relayed(k).start()

    pass_on(last)
    loop(last, pass_on)

    def settle(k):
        low(k).wait_recv()
        relayed(k).wait_recv()
        relayed(k).wait_send()

    loop(sp_count, settle)

    def sent(k):
        spread(k).wait_send()
        low(k).wait_send()
        high(k).wait_send()

    loop(last, sent)
    own_low().wait_send()
    own_high().wait_send()


def gather_blocks(block):
    sp_count, tp_count = lax.axis_size("sp"), lax.axis_size("tp")
    ring = pltpu.SemaphoreType.DMA((2, sp_count))
    return pl.pallas_call(
        functools.partial(gather_kernel, sp_count),
        out_shape=jax.ShapeDtypeStruct((sp_count, tp_count) + block.shape, block.dtype),
        in_specs=[IN_VMEM],
        out_specs=IN_VMEM,
        scratch_shapes=[ring, ring, ring, ring],
        compiler_params=comm_params(3),
    )(block)


LANES = 128


def attention_kernel(
    chunk, scale, me, query, latents, key_up, value_up, out, keys, values, top, total, summed
):
    rows, pairs = query.shape[0], summed.shape[0]
    latent_dim = value_up.shape[0]
    first_query = me[0] * rows
    top[...] = jnp.full_like(top, -1e30)
    total[...] = jnp.zeros_like(total)
    summed[...] = jnp.zeros_like(summed)
    left_half = lax.broadcasted_iota(jnp.int32, (rows, LANES), 1) < VALUE_DIM
    wide = 4 * LANES

    def one_chunk(j, carry):
        offset = pl.multiple_of(j * chunk, chunk)

        def key_columns(n, inner):
            columns = pl.ds(pl.multiple_of(n * wide, wide), wide)
            keys[:, columns] = jnp.dot(
                latents[pl.ds(offset, chunk), :],
                key_up[:, columns],
                preferred_element_type=jnp.float32,
            ).astype(jnp.bfloat16)
            return inner

        def value_columns(n, inner):
            columns = pl.ds(pl.multiple_of(n * wide, wide), wide)
            values[:, columns] = jnp.dot(
                latents[pl.ds(offset, chunk), :latent_dim],
                value_up[:, columns],
                preferred_element_type=jnp.float32,
            ).astype(jnp.bfloat16)
            return inner

        lax.fori_loop(0, keys.shape[1] // wide, key_columns, 0)
        lax.fori_loop(0, values.shape[1] // wide, value_columns, 0)

        def one_pair(p, inner):
            allowed = (
                offset + lax.broadcasted_iota(jnp.int32, (rows, chunk), 1)
            ) <= first_query + lax.broadcasted_iota(jnp.int32, (rows, chunk), 0)
            pair_values = values[:, pl.ds(pl.multiple_of(p * LANES, LANES), LANES)]
            factors, products = [], []
            for half in range(2):
                head = 2 * p + half
                columns = pl.ds(pl.multiple_of(head * LANES, LANES), LANES)
                scores = lax.dot_general(
                    query[:, columns],
                    keys[:, columns],
                    (((1,), (1,)), ((), ())),
                    preferred_element_type=jnp.float32,
                )
                scores = jnp.where(allowed, scores * scale, -1e30)
                before = top[head]
                newest = jnp.maximum(before, jnp.max(scores, axis=1, keepdims=True))
                factor = jnp.exp(before - newest)
                exponent = jnp.exp(scores - newest)
                top[head] = newest
                total[head] = total[head] * factor + jnp.sum(exponent, axis=1, keepdims=True)
                factors.append(factor)
                products.append(
                    jnp.dot(
                        exponent.astype(jnp.bfloat16),
                        pair_values,
                        preferred_element_type=jnp.float32,
                    )
                )
            summed[p] = summed[p] * jnp.where(left_half, factors[0], factors[1]) + jnp.where(
                left_half, products[0], products[1]
            )
            return inner

        lax.fori_loop(0, pairs, one_pair, 0)
        return carry

    lax.fori_loop(0, (first_query + rows - 1) // chunk + 1, one_chunk, 0)
    for p in range(pairs):
        divisor = jnp.where(left_half, total[2 * p], total[2 * p + 1])
        out[:, p * LANES : (p + 1) * LANES] = (summed[p] / divisor).astype(out.dtype)


def attend_all(query, latents, key_up, value_up, scale):
    rows = query.shape[0]
    heads = query.shape[1] // LANES
    chunk = math.gcd(latents.shape[0], 512)
    return pl.pallas_call(
        functools.partial(attention_kernel, chunk, scale),
        out_shape=jax.ShapeDtypeStruct((rows, value_up.shape[1]), jnp.bfloat16),
        in_specs=[pl.BlockSpec(memory_space=pltpu.SMEM)] + [IN_VMEM] * 4,
        out_specs=IN_VMEM,
        scratch_shapes=[
            pltpu.VMEM((chunk, key_up.shape[1]), jnp.bfloat16),
            pltpu.VMEM((chunk, value_up.shape[1]), jnp.bfloat16),
            pltpu.VMEM((heads, rows, 1), jnp.float32),
            pltpu.VMEM((heads, rows, 1), jnp.float32),
            pltpu.VMEM((heads // 2, rows, LANES), jnp.float32),
        ],
        compiler_params=pltpu.CompilerParams(vmem_limit_bytes=60 * 1024 * 1024),
    )(lax.axis_index("sp").astype(jnp.int32).reshape(1), query, latents, key_up, value_up)


def dispatch_table(normed_rows, route_rows, route_weights, experts, capacity):
    row_count = normed_rows.shape[0]
    flat_routes = route_rows.reshape(-1)
    onehot = (flat_routes[:, None] == jnp.arange(experts, dtype=jnp.int32)[None, :]).astype(
        jnp.int32
    )
    earlier = jnp.cumsum(onehot, axis=0) - onehot
    target = flat_routes * capacity + jnp.sum(earlier * onehot, axis=1)
    matches = (
        target.reshape(row_count, -1)[None, :, :]
        == jnp.arange(experts * capacity, dtype=jnp.int32)[:, None, None]
    )
    spread = jnp.any(matches, axis=2).astype(jnp.bfloat16)
    slot_table = jnp.dot(spread, normed_rows, preferred_element_type=jnp.float32).astype(
        jnp.bfloat16
    )
    combine = jnp.sum(jnp.where(matches, route_weights[None], 0.0), axis=2).T
    return (slot_table.reshape(experts, capacity, normed_rows.shape[1]), combine)


def on_device(
    query_nope,
    query_rope,
    latent,
    key_rope,
    latent_gain,
    key_up,
    value_up,
    out_proj,
    resid,
    attn_gain,
    pre_gain,
    routes,
    route_weights,
    expert_gate,
    expert_up,
    expert_down,
    shared_gate,
    shared_up,
    shared_down,
    moe_gain,
):
    local_rows = query_nope.shape[0]
    heads_here = query_nope.shape[1] // NOPE_DIM
    query_pos = lax.axis_index("sp") * local_rows + jnp.arange(local_rows, dtype=jnp.int32)
    query_rot = rotate(
        query_rope.astype(jnp.float32).reshape(local_rows, heads_here, ROPE_DIM), query_pos[:, None]
    ).astype(jnp.bfloat16)
    score_scale = (NOPE_DIM + ROPE_DIM) ** (-0.5)
    latent_dim = latent.shape[1]
    spare = LANES - NOPE_DIM - ROPE_DIM
    share = local_rows // lax.axis_size("tp")
    start = lax.axis_index("tp") * share
    share_pos = lax.axis_index("sp") * local_rows + start + jnp.arange(share, dtype=jnp.int32)
    latent_share = lax.dynamic_slice_in_dim(latent, start, share, 0)
    rope_share = lax.dynamic_slice_in_dim(key_rope, start, share, 0)
    block = jnp.concatenate(
        [
            rms_scale(latent_share.astype(jnp.float32), latent_gain).astype(jnp.bfloat16),
            rotate(rope_share.astype(jnp.float32), share_pos).astype(jnp.bfloat16),
            jnp.zeros((share, LANES - ROPE_DIM), jnp.bfloat16),
        ],
        axis=1,
    )
    latents = gather_blocks(block).reshape(-1, latent_dim + LANES)
    query = jnp.concatenate(
        [
            query_nope.reshape(local_rows, heads_here, NOPE_DIM),
            query_rot,
            jnp.zeros((local_rows, heads_here, spare), jnp.bfloat16),
        ],
        axis=2,
    ).reshape(local_rows, heads_here * LANES)
    pass_rotary = jnp.eye(LANES, LANES, NOPE_DIM, dtype=jnp.bfloat16) * (
        jnp.arange(LANES) < ROPE_DIM
    ).astype(jnp.bfloat16)[:, None]
    key_map = jnp.concatenate(
        [
            jnp.pad(
                key_up.reshape(latent_dim, heads_here, NOPE_DIM),
                ((0, 0), (0, 0), (0, LANES - NOPE_DIM)),
            ).reshape(latent_dim, heads_here * LANES),
            jnp.tile(pass_rotary, (1, heads_here)),
        ],
        axis=0,
    )
    attention = attend_all(query, latents, key_map, value_up, score_scale)
    rows_here = resid.shape[0]
    model_dim = resid.shape[1]
    piece = math.gcd(rows_here, 16)
    projected = tp_reduce(
        jnp.dot(attention, out_proj, preferred_element_type=jnp.float32)
        .astype(jnp.bfloat16)
        .reshape(2, 2, -1, piece, model_dim)
    ).reshape(rows_here, model_dim)
    mixed = (resid.astype(jnp.float32) + rms_scale(projected, attn_gain)).astype(jnp.bfloat16)
    normed = rms_scale(mixed.astype(jnp.float32), pre_gain).astype(jnp.bfloat16)
    experts = lax.axis_size("sp")
    capacity = max(2, 2 * rows_here * TOP_K // experts)
    own_table, combine = dispatch_table(normed, routes, route_weights, experts, capacity)
    column, group_normed = dispatch(own_table, normed)
    expert_out = expert_block(
        column.reshape(-1, model_dim), expert_gate[0], expert_up[0], expert_down[0]
    )
    shared_part = expert_block(
        group_normed.reshape(-1, model_dim), shared_gate, shared_up, shared_down
    )
    expert_rows, shared_sum = give_back(
        expert_out.reshape(2, 2, experts, capacity, model_dim),
        shared_part.reshape(2, 2, -1, piece, model_dim),
    )
    expert_rows = expert_rows.reshape(-1, model_dim)
    shared_out = shared_sum.reshape(rows_here, model_dim)
    upper = combine.astype(jnp.bfloat16)
    lower = (combine - upper.astype(jnp.float32)).astype(jnp.bfloat16)
    both = jnp.dot(
        jnp.concatenate([upper, lower], axis=0), expert_rows, preferred_element_type=jnp.float32
    )
    routed = both[:rows_here] + both[rows_here:]
    moe = shared_out + routed
    return (mixed.astype(jnp.float32) + rms_scale(moe, moe_gain)).astype(jnp.bfloat16)


def solution(mesh):
    in_specs = (
        P("sp", "tp"),
        P("sp", "tp"),
        P("sp", None),
        P("sp", None),
        P(),
        P(None, "tp"),
        P(None, "tp"),
        P("tp", None),
        P(("sp", "tp"), None),
        P(),
        P(),
        P(("sp", "tp"), None),
        P(("sp", "tp"), None),
        P("sp", None, "tp"),
        P("sp", None, "tp"),
        P("sp", "tp", None),
        P(None, "tp"),
        P(None, "tp"),
        P("tp", None),
        P(),
    )
    out_specs = P(("sp", "tp"), None)
    return jax.shard_map(
        on_device, mesh=mesh, in_specs=in_specs, out_specs=out_specs, check_vma=False
    )
```
